32 devices in a mesh: sp: 4 (over y, x), tp: 8 (over z, core).
Axes of the slice: x: 2, y: 2, z: 4, core: 2. Of those that a mesh axis runs over, the one named last changes fastest.
Arguments:
- query_input: bfloat16 [1024, 1024], P('tp', 'sp'), may hold values from -6 to 6
- key_input: bfloat16 [1024, 1024], P('tp', 'sp'), may hold values from -6 to 6
- retrieved_content_matrix: bfloat16 [1024, 1024], P('tp', 'sp'), may hold values from -6 to 6
- gate_input: bfloat16 [1024, 1024], P('tp', 'sp'), may hold values from -6 to 6
- log_decay: float32 [2, 16, 1024], P(None, 'tp', 'sp'), may hold values from -2 to 0
- residual: bfloat16 [1024, 2048], P(('sp', 'tp')), may hold values from -6 to 6
- out_weight: bfloat16 [1024, 2048], replicated, may hold values from -0.1875 to 0.1875
- norm_gain: bfloat16 [2048], replicated, may hold values from 0.099609375 to 1.8984375
- routes: int32 [1024, 2], P(('sp', 'tp')), may hold values from 0 to 3, all different within a row; in each aligned block of 32 rows (0 to 31, 32 to 63, ...) at most 20 rows name the same one
- route_weight: float32 [1024, 2], P(('sp', 'tp')), may hold values from 0.1 to 1
- gate_weight: bfloat16 [4, 2048, 5504], P('sp', None, 'tp'), may hold values from -0.125 to 0.125
- up_weight: bfloat16 [4, 2048, 5504], P('sp', None, 'tp'), may hold values from -0.125 to 0.125
- down_weight: bfloat16 [4, 5504, 2048], P('sp', 'tp'), may hold values from -0.078125 to 0.078125
Outputs:
- output: bfloat16 [1024, 2048], P(('sp', 'tp'))
The draws below stay inside these ranges and needn't reach their ends.
Inputs may be any that keep to these rules, and one draw needn't show every extreme that they name: `routes`: each row names 2 different experts. In each aligned block of 32 rows no expert is named by more than 20 rows, a bound that some block reaches.
All inputs are finite; a program needn't handle non-finite values.
Results may differ from the reference program's by a relative error of at most 0.015.
Values may be sent and summed in bfloat16 or wider, within the bound.
A program may use at most 64 MiB of HBM per device.

```python
import math
import jax
import jax.numpy as jnp
import numpy as np
from jax import lax

D = 2048
HEADS = 16
HEAD_DIM = 64
RET_W = 1024
FF = 5504
FF_DEV = 688
EXPERTS = 4
TOP = 2
TOK_DEV = 256
TOK_TP = 32
TOKENS = 1024
CAP = 20
N_TP = 8


def draw_log_decay(key, part):
    streams = jax.random.split(key, 9)
    blocks = TOKENS // TOK_DEV
    sluggish_tally = HEADS // 2
    order_forward = jax.random.permutation(streams[0], HEADS)
    order_backward = jax.random.permutation(streams[1], HEADS)
    slow = jnp.stack([order_forward < sluggish_tally, order_backward < sluggish_tally])
    slow_rate = jax.random.uniform(streams[2], (2, HEADS), jnp.float32, 0.15, 0.4) / TOKENS
    fast_rate = jax.random.uniform(streams[3], (2, HEADS), jnp.float32, 0.015, 0.03)
    rate = jnp.where(slow, slow_rate, fast_rate)
    parity = jax.random.randint(streams[4], (), 0, 2)
    signs = jnp.where((jnp.arange(blocks) + parity) % 2 == 0, 1.0, -1.0)
    levels = jax.random.uniform(streams[5], (2, 1, blocks), jnp.float32, 0.5, 1.0)
    factor = jnp.repeat(jnp.exp2(signs[None, None, :] * levels), TOK_DEV, axis=2)
    rough = jax.random.uniform(streams[6], (2, HEADS, TOKENS), jnp.float32, 0.5, 1.5)
    starting_displacement = -rate[:, :, None] * factor * rough
    bucket_locations = jax.random.randint(streams[7], (2, HEADS, 2), 0, TOKENS)
    portion_quantities = jax.random.uniform(streams[8], (2, HEADS, 2), jnp.float32, math.log(0.5), math.log(0.8))
    element_locations = jnp.arange(TOKENS)
    element_runs = jnp.sum(jnp.where(element_locations[None, None, None, :] == bucket_locations[..., None], portion_quantities[..., None], 0.0), axis=2)
    return (starting_displacement + element_runs).astype(jnp.float32)


def level_of(key, dims, shards, least, largest):
    loudness, own = 1.0, jax.random.fold_in(key, 6)
    for dim, shards_of in shards:
        steps = jnp.exp(jax.random.uniform(jax.random.fold_in(own, dim), (shards_of,), jnp.float32, least / len(shards), largest / len(shards)))
        loudness = loudness * jnp.repeat(steps, dims[dim] // shards_of).reshape([-1 if axis == dim else 1 for axis in range(len(dims))])
    return loudness


def assign_block(own_key, own, number, rows, number_of, top, most, lean):
    order = jax.random.permutation(own_key, number_of)
    crowded, usual = portions_of(number_of, rows * top, most, lean, True), portions_of(number_of, rows * top, most, lean, False)
    places = jnp.arange(number_of)

    def named(sizes, rotation):
        used = int((sizes > 0).sum())
        fixed = max(1, used // 4)
        shifted = fixed + (places - fixed + rotation * (used - fixed)) % max(1, number_of - fixed)
        return jnp.zeros((number_of,), jnp.int32).at[order[jnp.where(places < fixed, places, shifted)]].set(jnp.asarray(sizes, jnp.int32))

    sizes = jnp.where(number % 4 == 0, named(crowded, number // 4), named(usual, number - number // 4 - 1))
    mixed = jax.random.permutation(jax.random.fold_in(own, 3), number_of)
    giver, receiver = mixed[0:number_of // 2 * 2:2], mixed[1:number_of // 2 * 2:2]
    margin = jnp.minimum(sizes[giver] - 1, most - sizes[receiver]) // 2
    margin = jnp.where((giver == order[0]) | (receiver == order[0]) | (sizes[receiver] == 0), 0, jnp.maximum(margin, 0))
    shifted = jax.random.randint(jax.random.fold_in(own, 4), (number_of // 2,), 0, 1 << 20) % (margin + 1)
    sizes = sizes.at[giver].add(-shifted).at[receiver].add(shifted)
    members = jnp.searchsorted(jnp.cumsum(sizes), jnp.arange(rows * top), side="right").astype(jnp.int32)
    table = members.reshape(top, rows).T
    table = table[jax.random.permutation(jax.random.fold_in(own, 1), rows)]
    rotation = jax.random.randint(jax.random.fold_in(own, 2), (rows, 1), 0, top)
    return jnp.take_along_axis(table, (jnp.arange(top)[None, :] + rotation) % top, axis=1)


def portions_of(count, total, reach, lean, full):
    loads = [(1 << 20) // math.isqrt(standing ** lean) + 1 for standing in range(1, count + 1)]
    largest = reach if full else min(reach, max(-(-total // count), total * loads[0] // sum(loads)))
    least = 1 if total - largest >= count - 1 else 0
    counts, surplus = [largest] + [least] * (count - 1), total - largest - least * (count - 1)
    while surplus > 0:
        candidates = [i for i in range(1, count) if counts[i] < largest] or [i for i in range(1, count) if counts[i] < reach]
        pool, budget = sum([loads[i] for i in candidates]), surplus
        for i in candidates:
            extra = min(reach - counts[i], max(1, budget * loads[i] // pool), surplus)
            counts[i] = counts[i] + extra
            surplus = surplus - extra
    return np.array(counts)


def gaussian(stream_key, extent, spread, limit, shards=(), held_as=jnp.bfloat16):
    result = jax.random.normal(stream_key, extent, jnp.float32) * spread
    if len(shards) > 0:
        result = level_of(stream_key, extent, shards, -0.22, 0.18) * result
    return jnp.clip(result, min=-limit, max=limit).astype(held_as)


def setup_inputs(seed: int = 0) -> dict:
    splits = jax.random.split(jax.random.key(seed), 14)
    query_input = gaussian(splits[0], (RET_W, TOKENS), 1.0, 6.0, ((0, 8), (1, 4)))
    key_input = gaussian(splits[1], (RET_W, TOKENS), 1.0, 6.0, ((0, 8), (1, 4)))
    retrieved_content_matrix = gaussian(splits[2], (RET_W, TOKENS), 1.0, 6.0, ((0, 8), (1, 4)))
    gate_input = gaussian(splits[3], (RET_W, TOKENS), 1.0, 6.0, ((0, 8), (1, 4)))
    log_decay = draw_log_decay(jax.random.fold_in(splits[13], 71), 0)
    residual = gaussian(splits[5], (TOKENS, D), 1.0, 6.0, ((0, 32),))
    out_weight = gaussian(splits[6], (RET_W, D), RET_W ** -0.5, 0.1875)
    norm_gain = jnp.clip(1.0 + 0.18 * jax.random.normal(splits[7], (D,), jnp.float32), 0.099609375, 1.8984375).astype(jnp.bfloat16)
    routes_keys = jax.random.split(jax.random.fold_in(splits[8], 1), TOKENS // TOK_TP)
    routes_turns = jax.random.permutation(jax.random.fold_in(splits[8], 3), TOKENS // TOK_TP)
    routes = jax.vmap(lambda own, number: assign_block(jax.random.fold_in(splits[8], 2), own, number, TOK_TP, EXPERTS, TOP, CAP, 1))(routes_keys, routes_turns).reshape((TOKENS, TOP))
    route_weight = jnp.clip(0.1 + 0.9 * jax.random.uniform(splits[9], (TOKENS, TOP), jnp.float32) ** level_of(splits[9], (TOKENS, TOP), ((0, 32),), -0.2, 0.2), 0.1, 1.0)
    gate_weight = gaussian(splits[10], (EXPERTS, D, FF), D ** -0.5, 0.125, ((0, 4), (2, 8)))
    up_weight = gaussian(splits[11], (EXPERTS, D, FF), D ** -0.5, 0.125, ((0, 4), (2, 8)))
    down_weight = gaussian(splits[12], (EXPERTS, FF, D), FF ** -0.5, 0.078125, ((0, 4), (1, 8)))
    return {"query_input": query_input, "key_input": key_input, "retrieved_content_matrix": retrieved_content_matrix, "gate_input": gate_input, "log_decay": log_decay, "residual": residual, "out_weight": out_weight, "norm_gain": norm_gain, "routes": routes, "route_weight": route_weight, "gate_weight": gate_weight, "up_weight": up_weight, "down_weight": down_weight}


full_precision = lax.Precision.HIGHEST

def head_norm(values, mesh_axis):
    centred = values - lax.optimization_barrier(jnp.mean(values, axis=mesh_axis, keepdims=True))
    return centred * lax.rsqrt(lax.optimization_barrier(jnp.mean(centred * centred, axis=mesh_axis, keepdims=True)) + 1e-06)

def reference(query_input, key_input, retrieved_content_matrix, gate_input, log_decay, residual, out_weight, norm_gain, routes, route_weight, gate_weight, up_weight, down_weight):
    segment_count = TOKENS // TOK_DEV

    def by_segment(array):
        shaped = array.astype(jnp.float32).reshape(HEADS, HEAD_DIM, segment_count, TOK_DEV)
        return jnp.transpose(shaped, (2, 0, 1, 3))
    queries = by_segment(query_input)
    all_keys = by_segment(key_input)
    all_values = by_segment(retrieved_content_matrix)
    gate_values = by_segment(gate_input)
    forward_log = jnp.transpose(log_decay[0].reshape(HEADS, segment_count, TOK_DEV), (1, 0, 2))
    backward_log = jnp.transpose(log_decay[1].reshape(HEADS, segment_count, TOK_DEV), (1, 0, 2))
    forward_prefix = jnp.cumsum(forward_log, axis=-1)
    backward_prefix = jnp.cumsum(backward_log, axis=-1) - backward_log
    forward_total = forward_prefix[..., -1]
    backward_total = lax.optimization_barrier(jnp.sum(backward_log, axis=-1))
    forward_keys = all_keys * jnp.exp(forward_total[..., None] - forward_prefix)[:, :, None, :]
    backward_keys = all_keys * jnp.exp(backward_prefix)[:, :, None, :]
    local_forward = jnp.einsum('nhds,nhes->nhde', forward_keys, all_values, precision=full_precision)
    backward_local = jnp.einsum('nhds,nhes->nhde', backward_keys, all_values, precision=full_precision)

    def carry_step(state, inputs):
        total, local = inputs
        return (jnp.exp(total)[:, None, None] * state + local, state)
    zero_state = jnp.zeros((HEADS, HEAD_DIM, HEAD_DIM), jnp.float32)
    _, forward_in = lax.scan(carry_step, zero_state, (forward_total, local_forward))
    _, backward_in = lax.scan(carry_step, zero_state, (backward_total, backward_local), reverse=True)
    offsets = jnp.arange(TOK_DEV)
    lower = offsets[:, None] >= offsets[None, :]
    upper = offsets[:, None] <= offsets[None, :]

    def segment_output(inputs):
        query_part, key_part, value_part, forward_part, backward_part, backward_sum, state_fwd, state_bwd = inputs
        scores = jnp.einsum('hdt,hds->hts', query_part, key_part)
        forward_decay_weight = jnp.exp(jnp.where(lower, forward_part[:, :, None] - forward_part[:, None, :], -jnp.inf))
        backward_weight = jnp.exp(jnp.where(upper, backward_part[:, None, :] - backward_part[:, :, None], -jnp.inf))
        weighted = (scores * (forward_decay_weight + backward_weight)).astype(jnp.bfloat16)
        weighted = lax.optimization_barrier(weighted).astype(jnp.float32)
        inner = jnp.einsum('hts,hes->het', weighted, value_part)
        carried = jnp.einsum('hdt,hde->het', query_part, state_fwd, precision=full_precision) * jnp.exp(forward_part)[:, None, :]
        carried = carried + jnp.einsum('hdt,hde->het', query_part, state_bwd, precision=full_precision) * jnp.exp(backward_sum[:, None] - backward_part)[:, None, :]
        return inner + carried
    retained = lax.map(segment_output, (queries, all_keys, all_values, forward_prefix, backward_prefix, backward_total, forward_in, backward_in))
    mixer_out = (head_norm(retained, 2) * jax.nn.silu(gate_values)).astype(jnp.bfloat16)
    mixer_tokens = jnp.transpose(mixer_out, (0, 3, 1, 2)).reshape(TOKENS, RET_W)
    stream = residual.astype(jnp.float32) + jnp.dot(mixer_tokens, out_weight, preferred_element_type=jnp.float32)
    scale = lax.rsqrt(lax.optimization_barrier(jnp.mean(stream * stream, axis=-1, keepdims=True)) + 1e-06)
    normed = (stream * scale * norm_gain.astype(jnp.float32)).astype(jnp.bfloat16)
    slots_total = CAP * (TOKENS // TOK_TP)

    def expert_step(expert, moe_sum):
        chosen = jnp.any(routes == expert, axis=-1)
        picked = jnp.nonzero(chosen, size=slots_total, fill_value=0)[0].astype(jnp.int32)
        valid = (jnp.arange(slots_total) < jnp.sum(chosen.astype(jnp.int32))).astype(jnp.float32)
        inputs = normed[picked]
        gates = jnp.dot(inputs, gate_weight[expert], preferred_element_type=jnp.float32)
        ups = jnp.dot(inputs, up_weight[expert], preferred_element_type=jnp.float32)
        hidden = (jax.nn.silu(gates) * ups).astype(jnp.bfloat16)
        grouped = hidden.reshape(slots_total, N_TP, FF_DEV).astype(jnp.float32)
        down_groups = down_weight[expert].reshape(N_TP, FF_DEV, D).astype(jnp.float32)
        parts = jnp.einsum('rjf,jfd->rjd', grouped, down_groups).astype(jnp.bfloat16)
        parts = lax.optimization_barrier(parts).astype(jnp.float32)
        expert_out = lax.optimization_barrier(jnp.sum(parts, axis=1)).astype(jnp.bfloat16)
        weight = lax.optimization_barrier(jnp.sum(jnp.where(routes[picked] == expert, route_weight[picked], 0.0), axis=-1)) * valid
        return moe_sum.at[picked].add(weight[:, None] * expert_out.astype(jnp.float32))
    moe_sum = lax.fori_loop(0, EXPERTS, expert_step, jnp.zeros((TOKENS, D), jnp.float32))
    return (stream + moe_sum).astype(jnp.bfloat16)
```

```python
import functools

import jax
import jax.numpy as jnp
from jax import lax
from jax.experimental import pallas as pl
from jax.experimental.pallas import tpu as pltpu
from jax.sharding import PartitionSpec as P

HEAD_DIM = 64
HIGH = lax.Precision.HIGHEST
F32 = jnp.float32
BF16 = jnp.bfloat16
NN = (((1,), (0,)), ((), ()))
NT = (((1,), (1,)), ((), ()))
TN = (((0,), (0,)), ((), ()))


def dot(a, b, dims=NN, precision=None):
    return lax.dot_general(a, b, dims, precision=precision, preferred_element_type=F32)


def kernel(
    n_sp, n_tp, slots,
    q_ref, k_ref, v_ref, g_ref, ld_ref, rt_ref, res_ref, ng_ref, wo_hbm, wg_hbm, wu_hbm, wd_hbm,
    out_ref,
    wo, wg, wu, wd, st, yg, res, rts, stream, normed, sel, xs, xr, pw, pr, rs, rr, zacc, zs, zr,
    wsem, st_s, st_r, y_s, y_r, res_s, res_r, rt_s, rt_r, x_s, x_r, f_s, f_r, p_s, p_r, b_s, b_r, z_s, z_r,
):
    sp, tp = lax.axis_index("sp"), lax.axis_index("tp")
    chips = n_tp // 2
    chip, core = tp // 2, lax.rem(tp, 2)
    partner = chip * 2 + 1 - core
    feats, length = q_ref.shape
    heads = feats // HEAD_DIM
    tok = res_ref.shape[0]
    half = wo.shape[1] // 2

    def remote(src, dst, send, recv, to_sp, to_tp):
        return pltpu.make_async_remote_copy(
            src_ref=src, dst_ref=dst, send_sem=send, recv_sem=recv,
            device_id=(to_sp, to_tp), device_id_type=pl.DeviceIdType.MESH,
        )

    loads = []
    for i, (a, b) in enumerate(((wo_hbm, wo), (wg_hbm.at[0], wg), (wu_hbm.at[0], wu), (wd_hbm.at[0], wd))):
        loads.append(pltpu.make_async_copy(a, b, wsem.at[i]))
        loads[-1].start()

    barrier = pltpu.get_barrier_semaphore()
    for d in range(1, n_tp):
        pl.semaphore_signal(barrier, inc=1, device_id=(sp, lax.rem(tp + d, n_tp)), device_id_type=pl.DeviceIdType.MESH)
    for d in range(1, n_sp):
        pl.semaphore_signal(barrier, inc=1, device_id=(lax.rem(sp + d, n_sp), tp), device_id_type=pl.DeviceIdType.MESH)

    def slot_tp(d, c):
        return lax.rem(chip + d + chips, chips) * 2 + c

    def gather_start(at, own, send, recv):
        for d in range(1, chips):
            remote(own, at(tp), send.at[d - 1], recv.at[tp], sp, slot_tp(d, core)).start()
        remote(own, at(tp), send.at[chips - 1], recv.at[tp], sp, partner).start()

    def gather_forward(at, own, send, recv):
        for d in range(1, chips):
            source = slot_tp(-d, core)
            remote(own, at(source), send.at[d - 1], recv.at[source], sp, partner).wait_recv()
            remote(at(source), at(source), send.at[chips - 1 + d], recv.at[source], sp, partner).start()

    def gather_finish(at, own, send, recv):
        for d in range(chips):
            source = slot_tp(-d, 1 - core)
            remote(own, at(source), send.at[d], recv.at[source], sp, partner).wait_recv()

    def gather_drain(at, own, send, recv):
        for d in range(2 * chips - 1):
            remote(own, at(tp), send.at[d], recv.at[tp], sp, partner).wait_send()

    def res_at(i):
        return res.at[pl.ds(pl.multiple_of(i * tok, tok), tok)]

    def y_at(i):
        return yg.at[pl.ds(pl.multiple_of(i * feats, feats), feats)]

    pl.semaphore_wait(barrier, n_tp - 1 + n_sp - 1)
    res_args = (res_at, res_ref, res_s, res_r)
    gather_start(*res_args)
    rt_copies = []
    for d in range(1, n_tp):
        to = lax.rem(tp + d, n_tp)
        c = remote(rt_ref, rts.at[tp], rt_s.at[d - 1], rt_r.at[tp], sp, to)
        c.start()
        rt_copies.append(c)
    rts[tp] = rt_ref[...]
    res[pl.ds(pl.multiple_of(tp * tok, tok), tok)] = res_ref[...]

    row = lax.broadcasted_iota(jnp.int32, (length, length), 0)
    col = lax.broadcasted_iota(jnp.int32, (length, length), 1)
    ld = ld_ref[...]
    upto = dot(ld, (row <= col).astype(F32), precision=HIGH)
    before = upto - ld
    upto_t, before_t = upto.T, before.T
    lane = lax.broadcasted_iota(jnp.int32, (8, 2 * HEAD_DIM), 1)
    for h in range(heads):
        cf, eb = upto[h:h + 1], before[heads + h:heads + h + 1]
        a_sum, b_sum = upto[h:h + 1, length - 1:], upto[heads + h:heads + h + 1, length - 1:]
        keys = k_ref[h * HEAD_DIM:(h + 1) * HEAD_DIM].astype(F32)
        values = v_ref[h * HEAD_DIM:(h + 1) * HEAD_DIM].astype(F32)
        both = jnp.concatenate([keys * jnp.exp(a_sum - cf), keys * jnp.exp(eb)], axis=0)
        st[sp, h, 0:HEAD_DIM] = dot(values, both, NT, HIGH)
        st[sp, h, HEAD_DIM:HEAD_DIM + 8] = jnp.where(lane < HEAD_DIM, a_sum, b_sum)
    st_copies = []
    for d in range(1, n_sp):
        to = lax.rem(sp + d, n_sp)
        c = remote(st.at[sp], st.at[sp], st_s.at[d - 1], st_r.at[sp], to, tp)
        c.start()
        st_copies.append(c)

    inner = []
    for h in range(heads):
        rows = slice(h * HEAD_DIM, (h + 1) * HEAD_DIM)
        scores = dot(q_ref[rows], k_ref[rows], TN)
        cf, cf_t = upto[h:h + 1], upto_t[:, h:h + 1]
        eb, eb_t = before[heads + h:heads + h + 1], before_t[:, heads + h:heads + h + 1]
        weight = jnp.exp(jnp.where(row >= col, cf_t - cf, -jnp.inf))
        weight = weight + jnp.exp(jnp.where(row <= col, eb - eb_t, -jnp.inf))
        inner.append(dot(v_ref[rows], (scores * weight).astype(BF16), NT))

    gather_forward(*res_args)
    for d in range(1, n_sp):
        source = lax.rem(sp + d, n_sp)
        remote(st.at[source], st.at[source], st_s.at[d - 1], st_r.at[source], source, tp).wait_recv()
    wide = lax.broadcasted_iota(jnp.int32, (1, 2 * HEAD_DIM), 1) < HEAD_DIM
    for h in range(heads):
        rows = slice(h * HEAD_DIM, (h + 1) * HEAD_DIM)
        cf, eb = upto[h:h + 1], before[heads + h:heads + h + 1]
        b_sum = upto[heads + h:heads + h + 1, length - 1:]
        totals = [st[m, h, HEAD_DIM:HEAD_DIM + 1] for m in range(n_sp)]
        state = jnp.zeros((HEAD_DIM, 2 * HEAD_DIM), F32)
        for m in range(n_sp):
            gap = jnp.zeros((1, 2 * HEAD_DIM), F32)
            for j in range(n_sp):
                if j > m:
                    gap = gap + jnp.where(wide & (j < sp), totals[j], 0.0)
                if j < m:
                    gap = gap + jnp.where(jnp.logical_not(wide) & (j > sp), totals[j], 0.0)
            used = (wide & (m < sp)) | (jnp.logical_not(wide) & (m > sp))
            state = state + jnp.where(used, jnp.exp(gap), 0.0) * st[m, h, 0:HEAD_DIM]
        queries = q_ref[rows].astype(F32)
        both = jnp.concatenate([queries * jnp.exp(cf), queries * jnp.exp(b_sum - eb)], axis=0)
        o = inner[h] + dot(state, both, NN, HIGH)
        o = o - jnp.mean(o, axis=0, keepdims=True)
        o = o * lax.rsqrt(jnp.mean(o * o, axis=0, keepdims=True) + 1e-06)
        gate = g_ref[rows].astype(F32)
        y = (o * (gate / (1.0 + jnp.exp(-gate)))).astype(BF16)
        yg[pl.ds(pl.multiple_of(tp * feats + h * HEAD_DIM, HEAD_DIM), HEAD_DIM)] = y
    y_args = (y_at, y_at(tp), y_s, y_r)
    gather_start(*y_args)

    for d in range(1, n_tp):
        source = lax.rem(tp + d, n_tp)
        remote(rt_ref, rts.at[source], rt_s.at[d - 1], rt_r.at[source], sp, source).wait_recv()
    info = rts[0]
    for j in range(1, n_tp):
        info = info + rts[j]
    experts = sel.shape[0]
    padded = (experts + 15) // 16 * 16
    expert = lax.broadcasted_iota(jnp.int32, (padded, length), 0).astype(F32)
    first, second = expert == info[0:1], expert == info[1:2]
    match = jnp.where(first | second, 1.0, 0.0)
    pair_weight = jnp.where(first, info[2:3], 0.0) + jnp.where(second, info[3:4], 0.0)
    rank = dot(match.astype(BF16), jnp.where(row < col, 1.0, 0.0).astype(BF16))
    place = lax.broadcasted_iota(jnp.int32, (slots, length), 0).astype(F32)
    slot_weight = []
    for e in range(experts):
        chosen = (place == rank[e:e + 1]) & (match[e:e + 1] > 0.0)
        sel[e] = jnp.where(chosen, 1.0, 0.0).astype(BF16)
        slot_weight.append(jnp.sum(jnp.where(chosen, pair_weight[e:e + 1], 0.0), axis=1, keepdims=True))

    gather_finish(*res_args)
    loads[0].wait()
    gather_forward(*y_args)
    gather_finish(*y_args)
    stream[...] = res[...].astype(F32) + dot(yg[...], wo[...], TN)
    s = stream[...]
    scale = lax.rsqrt(jnp.mean(s * s, axis=1, keepdims=True) + 1e-06)
    normed[...] = (s * scale * ng_ref[...].astype(F32)).astype(BF16)

    def x_copy(e, to, frm, send):
        return remote(xs.at[e, core], xr.at[frm, core], x_s.at[send], x_r.at[frm], to, tp)

    def dispatch(d, carry):
        e = lax.rem(sp + d, n_sp)
        for c in range(2):
            xs[e, c] = dot(sel[e], normed[:, c * half:(c + 1) * half]).astype(BF16)
        x_copy(e, e, sp, d - 1).start()
        return carry

    lax.fori_loop(1, n_sp, dispatch, 0)
    for c in range(2):
        xr[sp, c] = dot(sel[sp], normed[:, c * half:(c + 1) * half]).astype(BF16)
    for c in loads[1:]:
        c.wait()

    def f_copy(frm, part, send):
        return remote(xr.at[frm, part], xr.at[frm, part], f_s.at[send], f_r.at[frm], sp, partner)

    def p_copy(frm):
        return remote(pw.at[frm], pr.at[frm], p_s.at[frm], p_r.at[frm], sp, partner)

    def b_copy(frm, slot, send):
        return remote(rs.at[frm], rr.at[slot], b_s.at[send], b_r.at[slot], frm, tp)

    def expert_step(d, carry):
        frm = lax.rem(sp - d + n_sp, n_sp)

        @pl.when(d > 0)
        def _():
            x_copy(frm, frm, frm, d - 1).wait_recv()
            f_copy(frm, core, d - 1).start()
            f_copy(frm, 1 - core, d - 1).wait_recv()

        x0, x1 = xr[frm, 0], xr[frm, 1]
        gates = dot(x0, wg[0:half]) + dot(x1, wg[half:])
        ups = dot(x0, wu[0:half]) + dot(x1, wu[half:])
        hidden = (gates / (1.0 + jnp.exp(-gates)) * ups).astype(BF16)
        other = pl.multiple_of((1 - core) * half, half)
        mine = pl.multiple_of(core * half, half)
        pw[frm] = dot(hidden, wd[:, pl.ds(other, half)]).astype(BF16)
        p_copy(frm).start()
        kept = dot(hidden, wd[:, pl.ds(mine, half)])
        p_copy(frm).wait_recv()
        total = (kept + pr[frm].astype(F32)).astype(BF16)

        @pl.when(d > 0)
        def _():
            rs[frm] = total
            b_copy(frm, sp, d - 1).start()

        @pl.when(d == 0)
        def _():
            rr[sp] = total

        return carry

    lax.fori_loop(0, n_sp, expert_step, 0)

    for d in range(1, n_sp):
        source = lax.rem(sp + d, n_sp)
        b_copy(source, source, d - 1).wait_recv()
    for e in range(experts):
        weighted = (rr[e].astype(F32) * slot_weight[e]).astype(BF16)
        term = dot(sel[e], weighted, TN)
        if e == 0:
            zacc[...] = term
        else:
            zacc[...] += term
    zs[...] = zacc[...].astype(BF16)
    z_copies = []
    for d in range(1, n_tp):
        to = lax.rem(tp + d, n_tp)
        c = remote(zs.at[pl.ds(pl.multiple_of(to * tok, tok), tok)], zr.at[tp], z_s.at[d - 1], z_r.at[tp], sp, to)
        c.start()
        z_copies.append(c)
    own = pl.ds(pl.multiple_of(tp * tok, tok), tok)
    zr[tp] = zs[own]
    for d in range(1, n_tp):
        source = lax.rem(tp + d, n_tp)
        remote(zs.at[own], zr.at[source], z_s.at[d - 1], z_r.at[source], sp, source).wait_recv()
    for c in range(2):
        total = stream[own, c * half:(c + 1) * half]
        for i in range(chips):
            total = total + zr[2 * i + c].astype(F32)
        out_ref[:, c * half:(c + 1) * half] = total.astype(BF16)

    for c in rt_copies + st_copies + z_copies:
        c.wait_send()
    gather_drain(*res_args)
    gather_drain(*y_args)

    def drain(d, carry):
        frm = lax.rem(sp - d + n_sp, n_sp)
        p_copy(frm).wait_send()

        @pl.when(d > 0)
        def _():
            x_copy(frm, frm, frm, d - 1).wait_send()
            f_copy(frm, core, d - 1).wait_send()
            b_copy(frm, sp, d - 1).wait_send()

        return carry

    lax.fori_loop(0, n_sp, drain, 0)


def on_device(
    query_input, key_input, retrieved_content_matrix, gate_input, log_decay, residual, out_weight,
    norm_gain, routes, route_weight, gate_weight, up_weight, down_weight,
):
    n_sp, n_tp = lax.axis_size("sp"), lax.axis_size("tp")
    feats, length = query_input.shape
    heads = feats // HEAD_DIM
    tok, picks = routes.shape
    width = residual.shape[1]
    half = width // 2
    experts = n_sp * gate_weight.shape[0]
    ff = gate_weight.shape[2]
    capacity = (5 * tok + 2 * experts - 1) // (2 * experts)
    slots = (capacity * n_tp + 15) // 16 * 16
    ld = jnp.pad(log_decay.reshape(2 * heads, length), ((0, 8 - 2 * heads), (0, 0)))
    info = jnp.concatenate([routes.astype(F32).T, route_weight.T, jnp.zeros((4, tok), F32)], axis=0)
    mine = (jnp.arange(n_tp) == lax.axis_index("tp"))[None, :, None]
    rt = jnp.where(mine, info[:, None, :], 0.0).reshape(8, n_tp * tok)
    vm, dma = pltpu.VMEM, pltpu.SemaphoreType.DMA
    ns, nt = (n_sp,), (n_tp,)
    return pl.pallas_call(
        functools.partial(kernel, n_sp, n_tp, slots),
        out_shape=jax.ShapeDtypeStruct((tok, width), BF16),
        in_specs=[pl.BlockSpec(memory_space=vm)] * 8 + [pl.BlockSpec(memory_space=pl.ANY)] * 4,
        out_specs=pl.BlockSpec(memory_space=vm),
        scratch_shapes=[
            vm(out_weight.shape, BF16), vm((width, ff), BF16), vm((width, ff), BF16), vm((ff, width), BF16),
            vm((n_sp, heads, HEAD_DIM + 8, 2 * HEAD_DIM), F32),
            vm((n_tp * feats, length), BF16),
            vm((n_tp * tok, width), BF16),
            vm((n_tp, 8, length), F32),
            vm((length, width), F32), vm((length, width), BF16),
            vm((experts, slots, length), BF16),
            vm((n_sp, 2, slots, half), BF16), vm((n_sp, 2, slots, half), BF16),
            vm((n_sp, slots, half), BF16), vm((n_sp, slots, half), BF16),
            vm((n_sp, slots, half), BF16), vm((n_sp, slots, half), BF16),
            vm((length, half), F32), vm((length, half), BF16), vm((n_tp, tok, half), BF16),
            dma((4,)), dma(ns), dma(ns), dma(nt), dma(nt), dma(nt), dma(nt), dma(nt), dma(nt),
            dma(ns), dma(ns), dma(ns), dma(ns), dma(ns), dma(ns), dma(ns), dma(ns), dma(nt), dma(nt),
        ],
        compiler_params=pltpu.CompilerParams(
            collective_id=0, has_side_effects=True, vmem_limit_bytes=60 * 1024 * 1024
        ),
    )(
        query_input, key_input, retrieved_content_matrix, gate_input, ld, rt, residual,
        norm_gain.reshape(1, -1), out_weight, gate_weight, up_weight, down_weight,
    )


def solution(mesh):
    placed = (
        P("tp", "sp"), P("tp", "sp"), P("tp", "sp"), P("tp", "sp"), P(None, "tp", "sp"),
        P(("sp", "tp"), None), P(), P(), P(("sp", "tp"), None), P(("sp", "tp"), None),
        P("sp", None, "tp"), P("sp", None, "tp"), P("sp", "tp", None),
    )
    return jax.shard_map(
        on_device, mesh=mesh, in_specs=placed, out_specs=P(("sp", "tp"), None), check_vma=False
    )
```

```python
import functools

import jax
import jax.numpy as jnp
from jax import lax
from jax.experimental import pallas as pl
from jax.experimental.pallas import tpu as pltpu
from jax.sharding import PartitionSpec as P

HEAD_DIM = 64
HIGH = lax.Precision.HIGHEST
F32 = jnp.float32
BF16 = jnp.bfloat16
NN = (((1,), (0,)), ((), ()))
NT = (((1,), (1,)), ((), ()))
TN = (((0,), (0,)), ((), ()))


def dot(a, b, dims=NN, precision=None):
    return lax.dot_general(a, b, dims, precision=precision, preferred_element_type=F32)


def kernel(
    n_sp, n_tp, slots,
    q_ref, k_ref, v_ref, g_ref, ld_ref, routes_ref, weights_ref, res_ref, ng_ref, wo_hbm, wg_hbm, wu_hbm, wd_hbm,
    out_ref,
    wo, wg, wu, wd, ld_all, rt_ref, st, yg, res, rts, stream, normed, sel, xs, xr, hid, kept, pw, pr, rs, rr, zacc, zs, zr,
    wsem, st_s, st_r, y_s, y_r, res_s, res_r, rt_s, rt_r, x_s, x_r, f_s, f_r, p_s, p_r, b_s, b_r, z_s, z_r,
):
    sp, tp = lax.axis_index("sp"), lax.axis_index("tp")
    chips = n_tp // 2
    chip, core = tp // 2, lax.rem(tp, 2)
    partner = chip * 2 + 1 - core
    feats, length = q_ref.shape
    heads = feats // HEAD_DIM
    tok = res_ref.shape[0]
    half = wo.shape[1] // 2
    quarter = half // 2

    def remote(src, dst, send, recv, to_sp, to_tp):
        return pltpu.make_async_remote_copy(
            src_ref=src, dst_ref=dst, send_sem=send, recv_sem=recv,
            device_id=(to_sp, to_tp), device_id_type=pl.DeviceIdType.MESH,
        )

    loads = []
    for i, (a, b) in enumerate(((wo_hbm, wo), (wg_hbm.at[0], wg), (wu_hbm.at[0], wu), (wd_hbm.at[0], wd))):
        loads.append(pltpu.make_async_copy(a, b, wsem.at[i]))
        loads[-1].start()

    barrier = pltpu.get_barrier_semaphore()
    for d in range(1, n_tp):
        pl.semaphore_signal(barrier, inc=1, device_id=(sp, lax.rem(tp + d, n_tp)), device_id_type=pl.DeviceIdType.MESH)
    for d in range(1, n_sp):
        pl.semaphore_signal(barrier, inc=1, device_id=(lax.rem(sp + d, n_sp), tp), device_id_type=pl.DeviceIdType.MESH)

    def slot_tp(d, c):
        return lax.rem(chip + d + chips, chips) * 2 + c

    def gather_start(at, own, send, recv):
        for d in range(1, chips):
            remote(own, at(tp), send.at[d - 1], recv.at[tp], sp, slot_tp(d, core)).start()
        remote(own, at(tp), send.at[chips - 1], recv.at[tp], sp, partner).start()

    def gather_forward(at, own, send, recv):
        for d in range(1, chips):
            source = slot_tp(-d, core)
            remote(own, at(source), send.at[d - 1], recv.at[source], sp, partner).wait_recv()
            remote(at(source), at(source), send.at[chips - 1 + d], recv.at[source], sp, partner).start()

    def gather_finish(at, own, send, recv):
        for d in range(chips):
            source = slot_tp(-d, 1 - core)
            remote(own, at(source), send.at[d], recv.at[source], sp, partner).wait_recv()

    def gather_drain(at, own, send, recv):
        for d in range(2 * chips - 1):
            remote(own, at(tp), send.at[d], recv.at[tp], sp, partner).wait_send()

    def res_at(i):
        return res.at[pl.ds(pl.multiple_of(i * tok, tok), tok)]

    def y_at(i):
        return yg.at[pl.ds(pl.multiple_of(i * feats, feats), feats)]

    ld_all[...] = jnp.zeros_like(ld_all)
    ld_all[0:heads] = ld_ref[0]
    ld_all[heads:2 * heads] = ld_ref[1]
    token = lax.broadcasted_iota(jnp.int32, (tok, length), 0) + tp * tok
    spread = jnp.where(token == lax.broadcasted_iota(jnp.int32, (tok, length), 1), 1.0, 0.0)
    rt_ref[...] = jnp.zeros_like(rt_ref)
    rt_ref[0:2] = dot(routes_ref[...].astype(F32), spread, NN, HIGH)
    rt_ref[2:4] = dot(weights_ref[...], spread, NN, HIGH)
    pl.semaphore_wait(barrier, n_tp - 1 + n_sp - 1)
    res_args = (res_at, res_ref, res_s, res_r)
    gather_start(*res_args)
    rt_copies = []
    for d in range(1, n_tp):
        to = lax.rem(tp + d, n_tp)
        c = remote(rt_ref, rts.at[tp], rt_s.at[d - 1], rt_r.at[tp], sp, to)
        c.start()
        rt_copies.append(c)
    rts[tp] = rt_ref[...]
    res[pl.ds(pl.multiple_of(tp * tok, tok), tok)] = res_ref[...]

    row = lax.broadcasted_iota(jnp.int32, (length, length), 0)
    col = lax.broadcasted_iota(jnp.int32, (length, length), 1)
    ld = ld_all[...]
    upto = dot(ld, (row <= col).astype(F32), precision=HIGH)
    before = upto - ld
    upto_t, before_t = upto.T, before.T
    lane = lax.broadcasted_iota(jnp.int32, (8, 2 * HEAD_DIM), 1)
    for h in range(heads):
        cf, eb = upto[h:h + 1], before[heads + h:heads + h + 1]
        a_sum, b_sum = upto[h:h + 1, length - 1:], upto[heads + h:heads + h + 1, length - 1:]
        keys = k_ref[h * HEAD_DIM:(h + 1) * HEAD_DIM].astype(F32)
        values = v_ref[h * HEAD_DIM:(h + 1) * HEAD_DIM].astype(F32)
        both = jnp.concatenate([keys * jnp.exp(a_sum - cf), keys * jnp.exp(eb)], axis=0)
        st[sp, h, 0:HEAD_DIM] = dot(values, both, NT, HIGH)
        st[sp, h, HEAD_DIM:HEAD_DIM + 8] = jnp.where(lane < HEAD_DIM, a_sum, b_sum)
    st_copies = []
    for d in range(1, n_sp):
        to = lax.rem(sp + d, n_sp)
        c = remote(st.at[sp], st.at[sp], st_s.at[d - 1], st_r.at[sp], to, tp)
        c.start()
        st_copies.append(c)

    inner = []
    for h in range(heads):
        rows = slice(h * HEAD_DIM, (h + 1) * HEAD_DIM)
        scores = dot(q_ref[rows], k_ref[rows], TN)
        cf, cf_t = upto[h:h + 1], upto_t[:, h:h + 1]
        eb, eb_t = before[heads + h:heads + h + 1], before_t[:, heads + h:heads + h + 1]
        weight = jnp.exp(jnp.where(row >= col, cf_t - cf, -jnp.inf))
        weight = weight + jnp.exp(jnp.where(row <= col, eb - eb_t, -jnp.inf))
        inner.append(dot(v_ref[rows], (scores * weight).astype(BF16), NT))

    for d in range(1, n_sp):
        source = lax.rem(sp + d, n_sp)
        remote(st.at[source], st.at[source], st_s.at[d - 1], st_r.at[source], source, tp).wait_recv()
    wide = lax.broadcasted_iota(jnp.int32, (1, 2 * HEAD_DIM), 1) < HEAD_DIM
    for h in range(heads):
        rows = slice(h * HEAD_DIM, (h + 1) * HEAD_DIM)
        cf, eb = upto[h:h + 1], before[heads + h:heads + h + 1]
        b_sum = upto[heads + h:heads + h + 1, length - 1:]
        totals = [st[m, h, HEAD_DIM:HEAD_DIM + 1] for m in range(n_sp)]
        state = jnp.zeros((HEAD_DIM, 2 * HEAD_DIM), F32)
        for m in range(n_sp):
            gap = jnp.zeros((1, 2 * HEAD_DIM), F32)
            for j in range(n_sp):
                if j > m:
                    gap = gap + jnp.where(wide & (j < sp), totals[j], 0.0)
                if j < m:
                    gap = gap + jnp.where(jnp.logical_not(wide) & (j > sp), totals[j], 0.0)
            used = (wide & (m < sp)) | (jnp.logical_not(wide) & (m > sp))
            state = state + jnp.where(used, jnp.exp(gap), 0.0) * st[m, h, 0:HEAD_DIM]
        queries = q_ref[rows].astype(F32)
        both = jnp.concatenate([queries * jnp.exp(cf), queries * jnp.exp(b_sum - eb)], axis=0)
        o = inner[h] + dot(state, both, NN, HIGH)
        o = o - jnp.mean(o, axis=0, keepdims=True)
        o = o * lax.rsqrt(jnp.mean(o * o, axis=0, keepdims=True) + 1e-06)
        gate = g_ref[rows].astype(F32)
        y = (o * (gate / (1.0 + jnp.exp(-gate)))).astype(BF16)
        yg[pl.ds(pl.multiple_of(tp * feats + h * HEAD_DIM, HEAD_DIM), HEAD_DIM)] = y
    y_args = (y_at, y_at(tp), y_s, y_r)
    gather_start(*y_args)
    gather_forward(*res_args)

    for d in range(1, n_tp):
        source = lax.rem(tp + d, n_tp)
        remote(rt_ref, rts.at[source], rt_s.at[d - 1], rt_r.at[source], sp, source).wait_recv()
    info = rts[0]
    for j in range(1, n_tp):
        info = info + rts[j]
    experts = sel.shape[0]
    padded = (experts + 15) // 16 * 16
    expert = lax.broadcasted_iota(jnp.int32, (padded, length), 0).astype(F32)
    first, second = expert == info[0:1], expert == info[1:2]
    match = jnp.where(first | second, 1.0, 0.0)
    pair_weight = jnp.where(first, info[2:3], 0.0) + jnp.where(second, info[3:4], 0.0)
    rank = dot(match.astype(BF16), jnp.where(row < col, 1.0, 0.0).astype(BF16))
    place = lax.broadcasted_iota(jnp.int32, (slots, length), 0).astype(F32)
    slot_weight = []
    for e in range(experts):
        chosen = (place == rank[e:e + 1]) & (match[e:e + 1] > 0.0)
        sel[e] = jnp.where(chosen, 1.0, 0.0).astype(BF16)
        slot_weight.append(jnp.sum(jnp.where(chosen, pair_weight[e:e + 1], 0.0), axis=1, keepdims=True))

    loads[0].wait()
    gather_forward(*y_args)
    gather_finish(*res_args)
    gather_finish(*y_args)
    stream[...] = res[...].astype(F32) + dot(yg[...], wo[...], TN)
    s = stream[...]
    scale = lax.rsqrt(jnp.mean(s * s, axis=1, keepdims=True) + 1e-06)
    normed[...] = (s * scale * ng_ref[...].astype(F32)[None, :]).astype(BF16)

    def x_copy(e, to, frm, send):
        return remote(xs.at[e], xr.at[frm, core], x_s.at[send], x_r.at[frm], to, tp)

    def dispatch(d, carry):
        e = lax.rem(sp + d, n_sp)
        xs[e] = dot(sel[e], normed[:, pl.ds(pl.multiple_of(core * half, half), half)]).astype(BF16)
        x_copy(e, e, sp, d - 1).start()
        return carry

    lax.fori_loop(1, n_sp, dispatch, 0)
    for c in range(2):
        xr[sp, c] = dot(sel[sp], normed[:, c * half:(c + 1) * half]).astype(BF16)
    for c in loads[1:]:
        c.wait()

    def f_copy(frm, part, send):
        return remote(xr.at[frm, part], xr.at[frm, part], f_s.at[send], f_r.at[frm], sp, partner)

    def p_copy(i):
        return remote(pw.at[i], pr.at[i], p_s.at[i], p_r.at[i], sp, partner)

    def b_copy(part, to, slot, send):
        i = part * n_sp
        return remote(rs.at[i + to], rr.at[i + slot], b_s.at[i + send], b_r.at[i + slot], to, tp)

    def give_back(d, part, hidden):
        frm = lax.rem(sp - d + n_sp, n_sp)
        i = part * n_sp + frm
        other = pl.multiple_of((1 - core) * half + part * quarter, quarter)
        mine = pl.multiple_of(core * half + part * quarter, quarter)
        pw[i] = dot(hidden, wd[:, pl.ds(other, quarter)]).astype(BF16)
        p_copy(i).start()
        kept[i] = dot(hidden, wd[:, pl.ds(mine, quarter)])

    def finish(d, part):
        frm = lax.rem(sp - d + n_sp, n_sp)
        i = part * n_sp + frm
        p_copy(i).wait_recv()
        total = (kept[i] + pr[i].astype(F32)).astype(BF16)

        @pl.when(d > 0)
        def _():
            rs[i] = total
            b_copy(part, frm, sp, d - 1).start()

        @pl.when(d == 0)
        def _():
            rr[i] = total

    def expert_step(d, carry):
        frm = lax.rem(sp - d + n_sp, n_sp)

        @pl.when(d > 0)
        def _():
            x_copy(frm, frm, frm, d - 1).wait_recv()
            f_copy(frm, core, d - 1).start()
            f_copy(frm, 1 - core, d - 1).wait_recv()

        x0, x1 = xr[frm, 0], xr[frm, 1]
        gates = dot(x0, wg[:, 0:half], NT) + dot(x1, wg[:, half:], NT)
        ups = dot(x0, wu[:, 0:half], NT) + dot(x1, wu[:, half:], NT)
        hidden = (gates / (1.0 + jnp.exp(-gates)) * ups).astype(BF16)
        hid[frm] = hidden
        give_back(d, 0, hidden)

        @pl.when(d > 0)
        def _():
            finish(d - 1, 0)

        return carry

    def second_step(d, carry):
        give_back(d, 1, hid[lax.rem(sp - d + n_sp, n_sp)])

        @pl.when(d == 0)
        def _():
            finish(n_sp - 1, 0)

        @pl.when(d > 0)
        def _():
            finish(d - 1, 1)

        return carry

    lax.fori_loop(0, n_sp, expert_step, 0)
    lax.fori_loop(0, n_sp, second_step, 0)
    finish(n_sp - 1, 1)

    own = pl.ds(pl.multiple_of(tp * tok, tok), tok)
    z_copies = []
    for part in range(2):
        for d in range(1, n_sp):
            source = lax.rem(sp + d, n_sp)
            b_copy(part, source, source, d - 1).wait_recv()
        for e in range(experts):
            weighted = (rr[part * n_sp + e].astype(F32) * slot_weight[e]).astype(BF16)
            term = dot(sel[e], weighted, TN)
            if e == 0:
                zacc[...] = term
            else:
                zacc[...] += term
        zs[part] = zacc[...].astype(BF16)
        for d in range(1, n_tp):
            to = lax.rem(tp + d, n_tp)
            c = remote(
                zs.at[part, pl.ds(pl.multiple_of(to * tok, tok), tok)], zr.at[part * n_tp + tp],
                z_s.at[part * n_tp + d - 1], z_r.at[part * n_tp + tp], sp, to,
            )
            c.start()
            z_copies.append(c)
        zr[part * n_tp + tp] = zs[part, own]
    for part in range(2):
        for d in range(1, n_tp):
            source = lax.rem(tp + d, n_tp)
            i = part * n_tp + source
            remote(zs.at[part, own], zr.at[i], z_s.at[part * n_tp + d - 1], z_r.at[i], sp, source).wait_recv()
        for c in range(2):
            columns = slice(c * half + part * quarter, c * half + (part + 1) * quarter)
            total = stream[own, columns]
            for i in range(chips):
                total = total + zr[part * n_tp + 2 * i + c].astype(F32)
            out_ref[:, columns] = total.astype(BF16)

    for c in rt_copies + st_copies + z_copies:
        c.wait_send()
    gather_drain(*res_args)
    gather_drain(*y_args)

    def drain(d, carry):
        frm = lax.rem(sp - d + n_sp, n_sp)
        p_copy(frm).wait_send()
        p_copy(n_sp + frm).wait_send()

        @pl.when(d > 0)
        def _():
            x_copy(frm, frm, frm, d - 1).wait_send()
            f_copy(frm, core, d - 1).wait_send()
            b_copy(0, frm, sp, d - 1).wait_send()
            b_copy(1, frm, sp, d - 1).wait_send()

        return carry

    lax.fori_loop(0, n_sp, drain, 0)


def on_device(
    query_input, key_input, retrieved_content_matrix, gate_input, log_decay, residual, out_weight,
    norm_gain, routes, route_weight, gate_weight, up_weight, down_weight,
):
    n_sp, n_tp = lax.axis_size("sp"), lax.axis_size("tp")
    feats, length = query_input.shape
    heads = feats // HEAD_DIM
    tok, picks = routes.shape
    width = residual.shape[1]
    half = width // 2
    experts = n_sp * gate_weight.shape[0]
    ff = gate_weight.shape[2]
    capacity = (5 * tok + 2 * experts - 1) // (2 * experts)
    slots = (capacity * n_tp + 15) // 16 * 16
    vm, dma = pltpu.VMEM, pltpu.SemaphoreType.DMA
    ns, nt = (n_sp,), (n_tp,)
    return pl.pallas_call(
        functools.partial(kernel, n_sp, n_tp, slots),
        out_shape=jax.ShapeDtypeStruct((tok, width), BF16),
        in_specs=[pl.BlockSpec(memory_space=vm)] * 9 + [pl.BlockSpec(memory_space=pl.ANY)] * 4,
        out_specs=pl.BlockSpec(memory_space=vm),
        scratch_shapes=[
            vm(out_weight.shape, BF16), vm((ff, width), BF16), vm((ff, width), BF16), vm((ff, width), BF16),
            vm((8, length), F32), vm((8, length), F32),
            vm((n_sp, heads, HEAD_DIM + 8, 2 * HEAD_DIM), F32),
            vm((n_tp * feats, length), BF16),
            vm((n_tp * tok, width), BF16),
            vm((n_tp, 8, length), F32),
            vm((length, width), F32), vm((length, width), BF16),
            vm((experts, slots, length), BF16),
            vm((n_sp, slots, half), BF16), vm((n_sp, 2, slots, half), BF16),
            vm((n_sp, slots, ff), BF16), vm((2 * n_sp, slots, half // 2), F32),
            vm((2 * n_sp, slots, half // 2), BF16), vm((2 * n_sp, slots, half // 2), BF16),
            vm((2 * n_sp, slots, half // 2), BF16), vm((2 * n_sp, slots, half // 2), BF16),
            vm((length, half // 2), F32), vm((2, length, half // 2), BF16), vm((2 * n_tp, tok, half // 2), BF16),
            dma((4,)), dma(ns), dma(ns), dma(nt), dma(nt), dma(nt), dma(nt), dma(nt), dma(nt),
            dma(ns), dma(ns), dma(ns), dma(ns), dma((2 * n_sp,)), dma((2 * n_sp,)),
            dma((2 * n_sp,)), dma((2 * n_sp,)), dma((2 * n_tp,)), dma((2 * n_tp,)),
        ],
        compiler_params=pltpu.CompilerParams(
            collective_id=0, has_side_effects=True, vmem_limit_bytes=60 * 1024 * 1024
        ),
    )(
        query_input, key_input, retrieved_content_matrix, gate_input, log_decay, routes.T, route_weight.T,
        residual,
        norm_gain, out_weight, jnp.swapaxes(gate_weight, 1, 2), jnp.swapaxes(up_weight, 1, 2),
        down_weight,
    )


def solution(mesh):
    placed = (
        P("tp", "sp"), P("tp", "sp"), P("tp", "sp"), P("tp", "sp"), P(None, "tp", "sp"),
        P(("sp", "tp"), None), P(), P(), P(("sp", "tp"), None), P(("sp", "tp"), None),
        P("sp", None, "tp"), P("sp", None, "tp"), P("sp", "tp", None),
    )
    return jax.shard_map(
        on_device, mesh=mesh, in_specs=placed, out_specs=P(("sp", "tp"), None), check_vma=False
    )
```
